32 devices in a mesh: sp: 16 (over z, x, core), tp: 2 (over y).
Axes of the slice: x: 2, y: 2, z: 4, core: 2. Of those that a mesh axis runs over, the one named last changes fastest.
Arguments:
- stream: bfloat16 [2048, 16384], P('tp', 'sp'), may hold values from -12 to 12
- norm_gain: float32 [2, 2048], P(None, 'tp'), may hold values from 0.1 to 1.9
- in_weight: bfloat16 [2, 2048, 1024], P(None, 'sp', 'tp'), may hold values from -0.125 to 0.125
- out_weight: bfloat16 [2, 1024, 2048], P(None, 'tp', 'sp'), may hold values from -0.1875 to 0.1875
- docs: int32 [16384], P('sp'), may hold values from 0 to 3, never falling along the last dimension, each value on 1 to 8192 neighbouring positions
Outputs:
- mixed_out: bfloat16 [2048, 16384], P('tp', 'sp')
The draws below stay inside these ranges and needn't reach their ends.
Inputs may be any that keep to these rules, and one draw needn't show every extreme that they name: `docs`: numbers never fall along the positions and start at 0; a document spans at most 8192 positions.
All inputs are finite; a program needn't handle non-finite values.
Results may differ from the reference program's by a relative error of at most 0.0095.
Values may be sent and summed in bfloat16 or wider, within the bound.
No kernel may reach another device: no remote copies, remote signals or barrier semaphores. Data moves between devices by JAX's collectives and lax.ppermute only.
A program may use at most 64 MiB of HBM per device.

```python
import math
import jax
import jax.numpy as jnp
import numpy as np
from jax import lax

D = 2048
PW = 1024
GROUPS = 4
WIDEST = 16
LAYERS = 2
TOKENS = 16384
DOCS = 4
DOC_MOST = 8192


def draw_stream(key, part):
    base_key, scale_key = jax.random.split(key)
    band_rows = D // 16
    base_draw = jnp.clip(jax.random.normal(base_key, (D, TOKENS), jnp.float32), -4.0, 4.0)
    levels = jnp.exp(jax.random.uniform(scale_key, (16, 1, 1), jnp.float32, jnp.log(0.3), jnp.log(3.0)))
    shaped = base_draw.reshape(16, band_rows, TOKENS) * levels
    return shaped.reshape(D, TOKENS).astype(jnp.bfloat16)


def steps_of(rng, shape, shards, low, high):
    factor_of, own = 1.0, jax.random.fold_in(rng, 6)
    for dim, shards_of in shards:
        steps = jnp.exp(jax.random.uniform(jax.random.fold_in(own, dim), (shards_of,), jnp.float32, low / len(shards), high / len(shards)))
        factor_of = factor_of * jnp.repeat(steps, shape[dim] // shards_of).reshape([-1 if axis == dim else 1 for axis in range(len(shape))])
    return factor_of


def split_up(amount, total, bound, skew):
    loads = [(1 << 20) // math.isqrt(grade ** skew) + 1 for grade in range(2, amount + 1)]
    rest, counts = total - bound - (amount - 1), [1] * (amount - 1)
    while rest > 0:
        candidates = [i for i in range(amount - 1) if counts[i] < bound]
        pool, left = sum([loads[i] for i in candidates]), rest
        for i in candidates:
            more = min(bound - counts[i], max(1, left * loads[i] // pool), rest)
            counts[i] = counts[i] + more
            rest = rest - more
    return np.array([bound] + counts)


def ragged(stream_key, count, total, limit, lean):
    if count == 2:
        one = jax.random.randint(stream_key, (), max(1, total - limit), min(limit, total - 1) + 1)
        return jnp.stack([one, total - one])
    lengths = jnp.asarray(split_up(count, total, limit, lean), jnp.int32)
    twos = (count - 1) // 2
    giver, taker = lengths[1:1 + 2 * twos:2], lengths[2:2 + 2 * twos:2]
    slack = jnp.minimum(giver - 1, limit - taker)
    moved = jax.random.randint(jax.random.fold_in(stream_key, 1), (twos,), 0, 1 << 20) % (slack + 1)
    lengths = lengths.at[1:1 + 2 * twos:2].set(giver - moved).at[2:2 + 2 * twos:2].set(taker + moved)
    return lengths[jax.random.permutation(jax.random.fold_in(stream_key, 2), count)]


def noise(stream_key, shape, scale, limit, cuts=(), kind=jnp.bfloat16):
    drawn = jax.random.normal(stream_key, shape, jnp.float32) * scale
    if len(cuts) > 0:
        drawn = steps_of(stream_key, shape, cuts, -0.22, 0.18) * drawn
    return jnp.clip(drawn, min=-limit, max=limit).astype(kind)


def setup_inputs(seed: int = 0) -> dict:
    streams_of = jax.random.split(jax.random.key(seed), 6)
    return {
        "stream": draw_stream(jax.random.fold_in(streams_of[5], 71), 0),
        "norm_gain": jnp.clip(1.0 + 0.18 * jax.random.normal(streams_of[1], (LAYERS, D), jnp.float32), 0.1, 1.9),
        "in_weight": noise(streams_of[2], (LAYERS, D, PW), D ** -0.5, 0.125, ((1, 16), (2, 2))),
        "out_weight": noise(streams_of[3], (LAYERS, PW, D), PW ** -0.5, 0.1875, ((1, 2), (2, 16))),
        "docs": jnp.searchsorted(jnp.cumsum(ragged(streams_of[4], DOCS, TOKENS, DOC_MOST, 1)), jnp.arange(TOKENS), side="right").astype(jnp.int32),
    }


def trailing_pool(values, docs, widths):
    length = values.shape[1]
    reach_back = WIDEST - 1
    extended = jnp.pad(values.astype(jnp.float32), ((0, 0), (reach_back, 0)))
    ext_docs = jnp.pad(docs + 1, (reach_back, 0))
    marker = docs + 1
    window_sum = jnp.zeros(values.shape, jnp.float32)
    members = jnp.zeros(values.shape, jnp.float32)
    for lag_step in range(WIDEST):
        lower_edge = reach_back - lag_step
        shifted = extended[:, lower_edge:lower_edge + length]
        same_doc = ext_docs[lower_edge:lower_edge + length] == marker
        inside = jnp.logical_and(same_doc[None, :], lag_step < widths[:, None])
        window_sum = window_sum + jnp.where(inside, shifted, jnp.float32(0.0))
        members = members + inside.astype(jnp.float32)
    return window_sum / members - values.astype(jnp.float32)

def reference(stream, norm_gain, in_weight, out_weight, docs):
    channel = lax.iota(jnp.int32, PW)
    widths = jnp.left_shift(jnp.int32(2), channel // (PW // GROUPS))
    residual = stream.astype(jnp.float32)
    for layer_idx in range(LAYERS):
        mean_square = lax.optimization_barrier(jnp.mean(residual * residual, axis=0))
        scaled = residual * lax.rsqrt(mean_square + 1e-06)[None, :] * norm_gain[layer_idx].astype(jnp.float32)[:, None]
        normed = scaled.astype(jnp.bfloat16)
        pool_in = jnp.dot(in_weight[layer_idx].T, normed, preferred_element_type=jnp.float32).astype(jnp.bfloat16)
        pooled = trailing_pool(pool_in, docs, widths).astype(jnp.bfloat16)
        residual = residual + jnp.dot(out_weight[layer_idx].T, pooled, preferred_element_type=jnp.float32)
    return residual.astype(jnp.bfloat16)
```

```python
import functools

import jax
import jax.numpy as jnp
from jax import lax
from jax.experimental import pallas as pl
from jax.experimental.pallas import tpu as pltpu
from jax.sharding import PartitionSpec as P

D = 2048
PW = 1024
GROUPS = 4
WIDEST = 16
LAYERS = 2
HALO = 128
BOTH = ("sp", "tp")

contract_rows = (((0,), (0,)), ((), ()))


def passed_along(block, axis, distance):
    devices = range(lax.axis_size(axis))
    route = [(i - distance, i) for i in devices if i - distance in devices]
    return lax.ppermute(block, axis, route)


def trailing_pool(values, docs_own, edge_values, edge_docs, widths):
    length = values.shape[1]
    reach_back = WIDEST - 1
    extended = jnp.concatenate([edge_values, values], axis=1).astype(jnp.float32)
    ext_docs = jnp.concatenate([edge_docs, docs_own + 1])
    marker = docs_own + 1
    window_sum = jnp.zeros(values.shape, jnp.float32)
    members = jnp.zeros(values.shape, jnp.float32)
    for lag_step in range(WIDEST):
        lower_edge = reach_back - lag_step
        shifted = lax.slice_in_dim(extended, lower_edge, lower_edge + length, axis=1)
        same_doc = lax.slice_in_dim(ext_docs, lower_edge, lower_edge + length) == marker
        inside = jnp.logical_and(same_doc[None, :], lag_step < widths[:, None])
        window_sum = window_sum + jnp.where(inside, shifted, jnp.float32(0.0))
        members = members + inside.astype(jnp.float32)
    return (window_sum / members - values.astype(jnp.float32)).astype(jnp.bfloat16)


def split_channels(stream, norm_gain, in_weight, out_weight, docs):
    local_rows, length = stream.shape
    pool_rows = in_weight.shape[2]
    channel = lax.axis_index("tp") * pool_rows + lax.iota(jnp.int32, pool_rows)
    widths = jnp.left_shift(jnp.int32(2), channel // (PW // GROUPS))
    residual = stream.astype(jnp.float32)
    for layer_idx in range(LAYERS):
        in_block, out_rows = (
            lax.all_gather(in_weight[layer_idx], "sp", axis=0, tiled=True),
            lax.all_gather(out_weight[layer_idx], "sp", axis=1, tiled=True),
        )
        squares = lax.psum(jnp.sum(residual * residual, axis=0), "tp")
        scaled = residual * lax.rsqrt(squares / D + 1e-06)[None, :] * norm_gain[layer_idx][:, None]
        normed = scaled.astype(jnp.bfloat16)
        pool_in = lax.dot_general(
            in_block,
            lax.all_gather(normed, "tp", axis=0, tiled=True),
            contract_rows,
            preferred_element_type=jnp.float32,
        ).astype(jnp.bfloat16)
        tail_from = length - WIDEST + 1
        edge_values, edge_docs = passed_along(
            (pool_in[:, tail_from:], docs[tail_from:] + 1), "sp", 1
        )
        pooled = trailing_pool(pool_in, docs, edge_values, edge_docs, widths)
        out_cols = lax.all_to_all(out_rows, "tp", split_axis=1, concat_axis=0, tiled=True)
        change = lax.dot_general(
            out_cols,
            lax.all_gather(pooled, "tp", axis=0, tiled=True),
            contract_rows,
            preferred_element_type=jnp.float32,
        )
        residual = residual + change
    return residual.astype(jnp.bfloat16)


def pieces_at(ids, pieces, target, sems, place):
    copies, k = [], 0
    for ref in pieces:
        for n in range(ref.shape[0]):
            copies.append(pltpu.make_async_copy(ref.at[n], place(target, ids[0, k], ids[1, k]), sems.at[k]))
            k += 1
    return copies


def in_kernel(ids, x_ref, gain_ref, docs_ref, *rest, parts, layer_first):
    pieces, (pooled_ref, w_buf, sems) = rest[:parts], rest[parts:]
    rows, cols = pieces[0].shape[1:]
    place = lambda target, i, j: target.at[pl.ds(pl.multiple_of(i * rows, rows), rows),
                                           pl.ds(pl.multiple_of(j * cols, cols), cols)]
    copies = pieces_at(ids, pieces, w_buf, sems, place)
    for copy in copies:
        copy.start()
    x = x_ref[...].astype(jnp.float32)
    mean_square = jnp.sum(x * x, axis=0, keepdims=True) / x.shape[0]
    normed = (x * lax.rsqrt(mean_square + 1e-06) * gain_ref[...]).astype(jnp.bfloat16)
    docs = docs_ref[...]
    wide = PW // GROUPS
    for copy in copies:
        copy.wait()
    same, members = {}, {}
    count = jnp.ones(docs.shape, jnp.float32)
    lag = 1
    for group in range(GROUPS):
        same[lag] = pltpu.roll(docs, lag, 1) == docs
        count = count + jnp.where(same[lag], pltpu.roll(count, lag, 1), 0.0)
        members[group] = 1.0 / count
        lag *= 2
    for group in range(GROUPS):
        chans = slice(group * wide, (group + 1) * wide)
        value = lax.dot_general(w_buf[:, chans], normed, contract_rows, preferred_element_type=jnp.float32)
        value = value.astype(jnp.bfloat16).astype(jnp.float32)
        total, lag = value, 1
        for _ in range(group + 1):
            total = total + jnp.where(same[lag], pltpu.roll(total, lag, 1), 0.0)
            lag *= 2
        pooled_ref[chans, :] = (total * members[group] - value).astype(jnp.bfloat16)


def out_kernel(ids, x_ref, pooled_ref, *rest, parts, skip):
    pieces, (r_ref, w_buf, sems) = rest[:parts], rest[parts:]
    rows, cols = pieces[0].shape[1:]
    place = lambda target, i, j: target.at[pl.ds(pl.multiple_of(j * rows, rows), rows),
                                           pl.ds(pl.multiple_of(i * cols, cols), cols)]
    copies = pieces_at(ids, pieces, w_buf, sems, place)
    for copy in copies:
        copy.start()
    pooled = pooled_ref[:, skip:]
    for copy in copies:
        copy.wait()
    step = 512
    for start in range(0, w_buf.shape[1], step):
        change = lax.dot_general(w_buf[:, start:start + step], pooled, contract_rows, preferred_element_type=jnp.float32)
        own = x_ref[start:start + step, skip:].astype(jnp.float32)
        r_ref[start:start + step, :] = (own + change).astype(r_ref.dtype)


def call(kernel, out, ids, blocks, pieces, scratch):
    vmem = pl.BlockSpec(memory_space=pltpu.VMEM)
    return pl.pallas_call(
        kernel,
        out_shape=out,
        in_specs=[pl.BlockSpec(memory_space=pltpu.SMEM)] + [vmem] * len(blocks)
        + [pl.BlockSpec(memory_space=pl.ANY)] * len(pieces),
        out_specs=vmem,
        scratch_shapes=[pltpu.VMEM(scratch, jnp.bfloat16), pltpu.SemaphoreType.DMA((ids.shape[1],))],
        compiler_params=pltpu.CompilerParams(vmem_limit_bytes=56 * 1024 * 1024),
    )(ids, *blocks, *pieces)


def gathered(block):
    return [lax.all_gather(block, BOTH)]


def gathered_ids():
    every = lax.iota(jnp.int32, lax.axis_size("sp") * lax.axis_size("tp"))
    return jnp.stack([every // lax.axis_size("tp"), every % lax.axis_size("tp")])


def split_tokens(stream, norm_gain, in_weight, out_weight, docs):
    length = stream.shape[1]
    own_len = length // 2
    half = lax.axis_index("tp")
    swap = lambda a: lax.ppermute(a, "tp", [(0, 1), (1, 0)])
    ids = gathered_ids()
    in_parts = [gathered(in_weight[layer]) for layer in range(LAYERS)]
    out_parts = [gathered(out_weight[layer]) for layer in range(LAYERS)]

    before = passed_along(stream[:, length - HALO:], "sp", 1)
    extended = jnp.concatenate([before, stream], axis=1)
    ext_docs = jnp.concatenate([passed_along(docs[length - HALO:] + 1, "sp", 1), docs + 1])
    span = own_len + HALO
    theirs = swap(lax.dynamic_slice_in_dim(extended, (1 - half) * own_len, span, axis=1))
    ours = lax.dynamic_slice_in_dim(extended, half * own_len, span, axis=1)
    first = half == 0
    x = jnp.concatenate([jnp.where(first, ours, theirs), jnp.where(first, theirs, ours)], axis=0)
    marks = lax.dynamic_slice_in_dim(ext_docs, half * own_len, span)[None, :]
    gain = lax.all_gather(norm_gain, "tp", axis=1, tiled=True)

    for layer in range(LAYERS):
        pooled = call(
            functools.partial(in_kernel, parts=len(in_parts[layer]), layer_first=layer == 0),
            jax.ShapeDtypeStruct((PW, span), jnp.bfloat16),
            ids, (x, gain[layer][:, None], marks), in_parts[layer], (D, PW))
        last = layer == LAYERS - 1
        skip = HALO if last else 0
        x = call(
            functools.partial(out_kernel, parts=len(out_parts[layer]), skip=skip),
            jax.ShapeDtypeStruct((D, span - skip), jnp.bfloat16 if last else jnp.float32),
            ids, (x, pooled), out_parts[layer], (PW, D))
    rows = D // 2
    kept = lax.dynamic_slice_in_dim(x, half * rows, rows, axis=0)
    got = swap(lax.dynamic_slice_in_dim(x, (1 - half) * rows, rows, axis=0))
    return jnp.concatenate([jnp.where(first, kept, got), jnp.where(first, got, kept)], axis=1)


def per_device(stream, norm_gain, in_weight, out_weight, docs):
    tokens_fit = lax.axis_size("tp") == 2 and stream.shape[1] % 256 == 0
    plan = split_tokens if tokens_fit else split_channels
    return plan(stream, norm_gain, in_weight, out_weight, docs)


def solution(mesh):
    return jax.shard_map(
        per_device,
        mesh=mesh,
        in_specs=(P("tp", "sp"), P(None, "tp"), P(None, "sp", "tp"), P(None, "tp", "sp"), P("sp")),
        out_specs=P("tp", "sp"),
        check_vma=False,
    )
```

```python
import functools

import jax
import jax.numpy as jnp
from jax import lax
from jax.experimental import pallas as pl
from jax.experimental.pallas import tpu as pltpu
from jax.sharding import PartitionSpec as P

D = 2048
PW = 1024
GROUPS = 4
WIDEST = 16
LAYERS = 2
HALO = 128
BOTH = ("sp", "tp")


contract_rows = (((0,), (0,)), ((), ()))


def passed_along(block, axis, distance):
    devices = range(lax.axis_size(axis))
    route = [(i - distance, i) for i in devices if i - distance in devices]
    return lax.ppermute(block, axis, route)


def trailing_pool(values, docs_own, edge_values, edge_docs, widths):
    length = values.shape[1]
    reach_back = WIDEST - 1
    extended = jnp.concatenate([edge_values, values], axis=1).astype(jnp.float32)
    ext_docs = jnp.concatenate([edge_docs, docs_own + 1])
    marker = docs_own + 1
    window_sum = jnp.zeros(values.shape, jnp.float32)
    members = jnp.zeros(values.shape, jnp.float32)
    for lag_step in range(WIDEST):
        lower_edge = reach_back - lag_step
        shifted = lax.slice_in_dim(extended, lower_edge, lower_edge + length, axis=1)
        same_doc = lax.slice_in_dim(ext_docs, lower_edge, lower_edge + length) == marker
        inside = jnp.logical_and(same_doc[None, :], lag_step < widths[:, None])
        window_sum = window_sum + jnp.where(inside, shifted, jnp.float32(0.0))
        members = members + inside.astype(jnp.float32)
    return (window_sum / members - values.astype(jnp.float32)).astype(jnp.bfloat16)


def split_channels(stream, norm_gain, in_weight, out_weight, docs):
    local_rows, length = stream.shape
    pool_rows = in_weight.shape[2]
    channel = lax.axis_index("tp") * pool_rows + lax.iota(jnp.int32, pool_rows)
    widths = jnp.left_shift(jnp.int32(2), channel // (PW // GROUPS))
    residual = stream.astype(jnp.float32)
    for layer_idx in range(LAYERS):
        in_block, out_rows = (
            lax.all_gather(in_weight[layer_idx], "sp", axis=0, tiled=True),
            lax.all_gather(out_weight[layer_idx], "sp", axis=1, tiled=True),
        )
        squares = lax.psum(jnp.sum(residual * residual, axis=0), "tp")
        scaled = residual * lax.rsqrt(squares / D + 1e-06)[None, :] * norm_gain[layer_idx][:, None]
        normed = scaled.astype(jnp.bfloat16)
        pool_in = lax.dot_general(
            in_block,
            lax.all_gather(normed, "tp", axis=0, tiled=True),
            contract_rows,
            preferred_element_type=jnp.float32,
        ).astype(jnp.bfloat16)
        tail_from = length - WIDEST + 1
        edge_values, edge_docs = passed_along(
            (pool_in[:, tail_from:], docs[tail_from:] + 1), "sp", 1
        )
        pooled = trailing_pool(pool_in, docs, edge_values, edge_docs, widths)
        out_cols = lax.all_to_all(out_rows, "tp", split_axis=1, concat_axis=0, tiled=True)
        change = lax.dot_general(
            out_cols,
            lax.all_gather(pooled, "tp", axis=0, tiled=True),
            contract_rows,
            preferred_element_type=jnp.float32,
        )
        residual = residual + change
    return residual.astype(jnp.bfloat16)


def pieces_at(ids, pieces, target, sems, place):
    copies, k = [], 0
    for ref in pieces:
        for n in range(ref.shape[0]):
            copies.append(pltpu.make_async_copy(ref.at[n], place(target, ids[0, k], ids[1, k]), sems.at[k]))
            k += 1
    return copies


def in_kernel(ids, x_ref, gain_ref, docs_ref, *rest, parts):
    pieces, (pooled_ref, w_buf, sems) = rest[:parts], rest[parts:]
    rows, cols = pieces[0].shape[1:]
    place = lambda target, i, j: target.at[pl.ds(pl.multiple_of(i * rows, rows), rows),
                                           pl.ds(pl.multiple_of(j * cols, cols), cols)]
    copies = pieces_at(ids, pieces, w_buf, sems, place)
    for copy in copies:
        copy.start()
    x = x_ref[...].astype(jnp.float32)
    mean_square = jnp.sum(x * x, axis=0, keepdims=True) / x.shape[0]
    normed = (x * lax.rsqrt(mean_square + 1e-06) * gain_ref[...]).astype(jnp.bfloat16)
    docs = docs_ref[...]
    wide = PW // GROUPS
    for copy in copies:
        copy.wait()
    same, members = {}, {}
    count = jnp.ones(docs.shape, jnp.float32)
    lag = 1
    for group in range(GROUPS):
        same[lag] = pltpu.roll(docs, lag, 1) == docs
        count = count + jnp.where(same[lag], pltpu.roll(count, lag, 1), 0.0)
        members[group] = 1.0 / count
        lag *= 2
    for group in range(GROUPS):
        chans = slice(group * wide, (group + 1) * wide)
        value = lax.dot_general(w_buf[:, chans], normed, contract_rows, preferred_element_type=jnp.float32)
        value = value.astype(jnp.bfloat16).astype(jnp.float32)
        total, lag = value, 1
        for _ in range(group + 1):
            total = total + jnp.where(same[lag], pltpu.roll(total, lag, 1), 0.0)
            lag *= 2
        pooled_ref[chans, :] = (total * members[group] - value).astype(jnp.bfloat16)


def out_kernel(ids, x_ref, pooled_ref, *rest, parts, skip, flip):
    pieces, (r_ref, w_buf, sems) = rest[:parts], rest[parts:]
    rows, cols = pieces[0].shape[1:]
    place = lambda target, i, j: target.at[pl.ds(pl.multiple_of(j * rows, rows), rows),
                                           pl.ds(pl.multiple_of(i * cols, cols), cols)]
    copies = pieces_at(ids, pieces, w_buf, sems, place)
    for copy in copies:
        copy.start()
    pooled = pooled_ref[:, skip:]
    for copy in copies:
        copy.wait()
    step = 512
    for start in range(0, r_ref.shape[0], step):
        at = start
        if flip is not None:
            at = pl.multiple_of((ids[2, 0] ^ flip) * r_ref.shape[0] + start, step)
        change = lax.dot_general(w_buf[:, pl.ds(at, step)], pooled, contract_rows, preferred_element_type=jnp.float32)
        own = x_ref[pl.ds(at, step), skip:].astype(jnp.float32)
        r_ref[start:start + step, :] = (own + change).astype(r_ref.dtype)


def call(kernel, out, ids, blocks, pieces, scratch):
    vmem = pl.BlockSpec(memory_space=pltpu.VMEM)
    return pl.pallas_call(
        kernel,
        out_shape=out,
        in_specs=[pl.BlockSpec(memory_space=pltpu.SMEM)] + [vmem] * len(blocks)
        + [pl.BlockSpec(memory_space=pl.ANY)] * len(pieces),
        out_specs=vmem,
        scratch_shapes=[pltpu.VMEM(scratch, jnp.bfloat16), pltpu.SemaphoreType.DMA((ids.shape[1],))],
        compiler_params=pltpu.CompilerParams(vmem_limit_bytes=56 * 1024 * 1024),
    )(ids, *blocks, *pieces)


def sent(block, dz=0, bx=0, by=0, bc=0):
    tp = lax.axis_size("tp")
    columns = lax.axis_size("sp") // 4
    route = []
    for n in range(4 * columns * tp):
        s, y = n // tp, n % tp
        z, x, c = s // 4, s // 2 % 2, s % 2
        to = ((z + dz) % columns * 4 + (x ^ bx) * 2 + (c ^ bc)) * tp + (y ^ by)
        route.append((n, to))
    return lax.ppermute(block, BOTH, route)


def lined_up(shard):
    columns = lax.axis_size("sp") // 4
    return jnp.stack([shard] + [sent(shard, dz=d) for d in range(1, columns)])


def after(value, earlier):
    return value if earlier is None else lax.optimization_barrier((value, earlier))[0]


def spread(line):
    cut = line.shape[0] // 4
    low, high = line[:cut], line[cut:]
    return line, low, high, sent(low, bx=1), sent(high, by=1)


def spread_on(blocks, two_before, one_before):
    line, low, high, low_x, high_y = blocks
    low_y = sent(after(jnp.concatenate([low, low_x]), two_before), by=1)
    high_x = sent(after(jnp.concatenate([high, high_y]), two_before), bx=1)
    near = jnp.concatenate([line, low_x, high_y])
    far = [after(block, one_before) for block in (low_y, high_x)]
    return [near, low_y, high_x] + [sent(block, bc=1) for block in (near, *far)]


def gathered_ids():
    tp = lax.axis_size("tp")
    columns = lax.axis_size("sp") // 4
    low, high = range(columns // 4), range(columns // 4, columns)
    own = [(d, 0, 0) for d in range(columns)] + [(d, 1, 0) for d in low] + [(d, 0, 1) for d in high]
    own += [(d, bx, 1) for bx in (0, 1) for d in low]
    own += [(d, 1, by) for by in (0, 1) for d in high]
    s, y = lax.axis_index("sp"), lax.axis_index("tp")
    dz, bx, by, bc = (jnp.array(v, jnp.int32) for v in zip(*[(*p, c) for c in (0, 1) for p in own]))
    z = (s // 4 - dz) % columns
    return jnp.stack([z * 4 + (s // 2 % 2 ^ bx) * 2 + (s % 2 ^ bc), y ^ by, jnp.full(dz.shape, y)])


def split_tokens(stream, norm_gain, in_weight, out_weight, docs):
    length = stream.shape[1]
    own_len = length // 2
    half = lax.axis_index("tp")
    first = half == 0
    swap = lambda a: sent(a, by=1)
    ids = gathered_ids()

    middle = stream[:, own_len - HALO:own_len]
    theirs = swap(lax.dynamic_slice_in_dim(stream, (1 - half) * own_len, own_len, axis=1))
    ours = lax.dynamic_slice_in_dim(stream, half * own_len, own_len, axis=1)

    shards = [block[layer] for layer in range(LAYERS) for block in (in_weight, out_weight)]
    weights, line = [], None
    for shard in shards:
        if line is not None:
            shard, line = lax.optimization_barrier((shard, line))
            weights.append(spread(line))
        line = lined_up(shard)
    weights.append(spread(line))

    before = passed_along(stream[:, length - HALO:], "sp", 1)
    our_edge = jnp.where(first, before, middle)
    their_edge = swap(jnp.where(first, middle, before))
    ext_docs = jnp.concatenate([passed_along(docs[length - HALO:] + 1, "sp", 1), docs + 1])
    span = own_len + HALO
    ours = jnp.concatenate([our_edge, ours], axis=1)
    theirs = jnp.concatenate([their_edge, theirs], axis=1)
    x = jnp.concatenate([jnp.where(first, ours, theirs), jnp.where(first, theirs, ours)], axis=0)
    marks = lax.dynamic_slice_in_dim(ext_docs, half * own_len, span)[None, :]
    other_gain = swap(norm_gain)
    gain = jnp.concatenate([jnp.where(first, norm_gain, other_gain), jnp.where(first, other_gain, norm_gain)], axis=1)

    done = [None, None]
    for layer in range(LAYERS):
        in_parts = spread_on(weights[2 * layer], *done[-2:])
        pooled = call(
            functools.partial(in_kernel, parts=len(in_parts)),
            jax.ShapeDtypeStruct((PW, span), jnp.bfloat16),
            ids, (x, gain[layer][:, None], marks), in_parts, (D, PW))
        done.append(pooled)
        out_parts = spread_on(weights[2 * layer + 1], *done[-2:])
        if layer < LAYERS - 1:
            x = call(
                functools.partial(out_kernel, parts=len(out_parts), skip=0, flip=None),
                jax.ShapeDtypeStruct((D, span), jnp.float32),
                ids, (x, pooled), out_parts, (PW, D))
            done.append(x)
    given, kept = [call(
        functools.partial(out_kernel, parts=len(out_parts), skip=HALO, flip=flip),
        jax.ShapeDtypeStruct((D // 2, own_len), jnp.bfloat16),
        ids, (x, pooled), out_parts, (PW, D)) for flip in (1, 0)]
    got = swap(given)
    out = jnp.zeros((D // 2, length), jnp.bfloat16)
    out = lax.dynamic_update_slice_in_dim(out, kept, half * own_len, axis=1)
    return lax.dynamic_update_slice_in_dim(out, got, (1 - half) * own_len, axis=1)


def per_device(stream, norm_gain, in_weight, out_weight, docs):
    tokens_fit = lax.axis_size("tp") == 2 and lax.axis_size("sp") % 16 == 0 and stream.shape[1] % 256 == 0
    plan = split_tokens if tokens_fit else split_channels
    return plan(stream, norm_gain, in_weight, out_weight, docs)


def solution(mesh):
    return jax.shard_map(
        per_device,
        mesh=mesh,
        in_specs=(P("tp", "sp"), P(None, "tp"), P(None, "sp", "tp"), P(None, "tp", "sp"), P("sp")),
        out_specs=P("tp", "sp"),
        check_vma=False,
    )
```

```python
import functools

import jax
import jax.numpy as jnp
from jax import lax
from jax.experimental import pallas as pl
from jax.experimental.pallas import tpu as pltpu
from jax.sharding import PartitionSpec as P

D = 2048
PW = 1024
GROUPS = 4
WIDEST = 16
LAYERS = 2
HALO = 128
BOTH = ("sp", "tp")


contract_rows = (((0,), (0,)), ((), ()))


def passed_along(block, axis, distance):
    devices = range(lax.axis_size(axis))
    route = [(i - distance, i) for i in devices if i - distance in devices]
    return lax.ppermute(block, axis, route)


def trailing_pool(values, docs_own, edge_values, edge_docs, widths):
    length = values.shape[1]
    reach_back = WIDEST - 1
    extended = jnp.concatenate([edge_values, values], axis=1).astype(jnp.float32)
    ext_docs = jnp.concatenate([edge_docs, docs_own + 1])
    marker = docs_own + 1
    window_sum = jnp.zeros(values.shape, jnp.float32)
    members = jnp.zeros(values.shape, jnp.float32)
    for lag_step in range(WIDEST):
        lower_edge = reach_back - lag_step
        shifted = lax.slice_in_dim(extended, lower_edge, lower_edge + length, axis=1)
        same_doc = lax.slice_in_dim(ext_docs, lower_edge, lower_edge + length) == marker
        inside = jnp.logical_and(same_doc[None, :], lag_step < widths[:, None])
        window_sum = window_sum + jnp.where(inside, shifted, jnp.float32(0.0))
        members = members + inside.astype(jnp.float32)
    return (window_sum / members - values.astype(jnp.float32)).astype(jnp.bfloat16)


def split_channels(stream, norm_gain, in_weight, out_weight, docs):
    local_rows, length = stream.shape
    pool_rows = in_weight.shape[2]
    channel = lax.axis_index("tp") * pool_rows + lax.iota(jnp.int32, pool_rows)
    widths = jnp.left_shift(jnp.int32(2), channel // (PW // GROUPS))
    residual = stream.astype(jnp.float32)
    for layer_idx in range(LAYERS):
        in_block, out_rows = (
            lax.all_gather(in_weight[layer_idx], "sp", axis=0, tiled=True),
            lax.all_gather(out_weight[layer_idx], "sp", axis=1, tiled=True),
        )
        squares = lax.psum(jnp.sum(residual * residual, axis=0), "tp")
        scaled = residual * lax.rsqrt(squares / D + 1e-06)[None, :] * norm_gain[layer_idx][:, None]
        normed = scaled.astype(jnp.bfloat16)
        pool_in = lax.dot_general(
            in_block,
            lax.all_gather(normed, "tp", axis=0, tiled=True),
            contract_rows,
            preferred_element_type=jnp.float32,
        ).astype(jnp.bfloat16)
        tail_from = length - WIDEST + 1
        edge_values, edge_docs = passed_along(
            (pool_in[:, tail_from:], docs[tail_from:] + 1), "sp", 1
        )
        pooled = trailing_pool(pool_in, docs, edge_values, edge_docs, widths)
        out_cols = lax.all_to_all(out_rows, "tp", split_axis=1, concat_axis=0, tiled=True)
        change = lax.dot_general(
            out_cols,
            lax.all_gather(pooled, "tp", axis=0, tiled=True),
            contract_rows,
            preferred_element_type=jnp.float32,
        )
        residual = residual + change
    return residual.astype(jnp.bfloat16)


def pieces_at(ids, pieces, target, sems, place):
    copies, k = [], 0
    for ref in pieces:
        for n in range(ref.shape[0]):
            copies.append(pltpu.make_async_copy(ref.at[n], place(target, ids[0, k], ids[1, k]), sems.at[k]))
            k += 1
    return copies


def in_kernel(ids, x_ref, gain_ref, docs_ref, *rest, parts):
    pieces, (pooled_ref, w_buf, sems) = rest[:parts], rest[parts:]
    rows, cols = pieces[0].shape[1:]
    place = lambda target, i, j: target.at[pl.ds(pl.multiple_of(i * rows, rows), rows),
                                           pl.ds(pl.multiple_of(j * cols, cols), cols)]
    copies = pieces_at(ids, pieces, w_buf, sems, place)
    for copy in copies:
        copy.start()
    x = x_ref[...].astype(jnp.float32)
    mean_square = jnp.sum(x * x, axis=0, keepdims=True) / x.shape[0]
    normed = (x * lax.rsqrt(mean_square + 1e-06) * gain_ref[...]).astype(jnp.bfloat16)
    docs = docs_ref[...]
    wide = PW // GROUPS
    for copy in copies:
        copy.wait()
    same, members = {}, {}
    count = jnp.ones(docs.shape, jnp.float32)
    lag = 1
    for group in range(GROUPS):
        same[lag] = pltpu.roll(docs, lag, 1) == docs
        count = count + jnp.where(same[lag], pltpu.roll(count, lag, 1), 0.0)
        members[group] = 1.0 / count
        lag *= 2
    for group in range(GROUPS):
        chans = slice(group * wide, (group + 1) * wide)
        value = lax.dot_general(w_buf[:, chans], normed, contract_rows, preferred_element_type=jnp.float32)
        value = value.astype(jnp.bfloat16).astype(jnp.float32)
        total, lag = value, 1
        for _ in range(group + 1):
            total = total + jnp.where(same[lag], pltpu.roll(total, lag, 1), 0.0)
            lag *= 2
        pooled_ref[chans, :] = (total * members[group] - value).astype(jnp.bfloat16)


def out_kernel(ids, x_ref, pooled_ref, *rest, parts, skip, flip):
    pieces, (r_ref, w_buf, sems) = rest[:parts], rest[parts:]
    rows, cols = pieces[0].shape[1:]
    place = lambda target, i, j: target.at[pl.ds(pl.multiple_of(j * rows, rows), rows),
                                           pl.ds(pl.multiple_of(i * cols, cols), cols)]
    copies = pieces_at(ids, pieces, w_buf, sems, place)
    for copy in copies:
        copy.start()
    pooled = pooled_ref[:, skip:]
    for copy in copies:
        copy.wait()
    step = 512
    for start in range(0, r_ref.shape[0], step):
        at = start
        if flip is not None:
            at = pl.multiple_of((ids[2, 0] ^ flip) * r_ref.shape[0] + start, step)
        change = lax.dot_general(w_buf[:, pl.ds(at, step)], pooled, contract_rows, preferred_element_type=jnp.float32)
        own = x_ref[pl.ds(at, step), skip:].astype(jnp.float32)
        r_ref[start:start + step, :] = (own + change).astype(r_ref.dtype)


def call(kernel, out, ids, blocks, pieces, scratch):
    vmem = pl.BlockSpec(memory_space=pltpu.VMEM)
    return pl.pallas_call(
        kernel,
        out_shape=out,
        in_specs=[pl.BlockSpec(memory_space=pltpu.SMEM)] + [vmem] * len(blocks)
        + [pl.BlockSpec(memory_space=pl.ANY)] * len(pieces),
        out_specs=vmem,
        scratch_shapes=[pltpu.VMEM(scratch, jnp.bfloat16), pltpu.SemaphoreType.DMA((ids.shape[1],))],
        compiler_params=pltpu.CompilerParams(vmem_limit_bytes=56 * 1024 * 1024),
    )(ids, *blocks, *pieces)


def sent(block, dz=0, bx=0, by=0, bc=0):
    tp = lax.axis_size("tp")
    columns = lax.axis_size("sp") // 4
    route = []
    for n in range(4 * columns * tp):
        s, y = n // tp, n % tp
        z, x, c = s // 4, s // 2 % 2, s % 2
        to = ((z + dz) % columns * 4 + (x ^ bx) * 2 + (c ^ bc)) * tp + (y ^ by)
        route.append((n, to))
    return lax.ppermute(block, BOTH, route)


def lined_up(shard):
    columns = lax.axis_size("sp") // 4
    return jnp.stack([shard] + [sent(shard, dz=d) for d in range(1, columns)])


def after(value, earlier):
    return value if earlier is None else lax.optimization_barrier((value, earlier))[0]


def spread(line):
    cut = line.shape[0] // 4
    low, high = line[:cut], line[cut:]
    return line, low, high, sent(low, bx=1), sent(high, by=1)


def spread_on(blocks, three_before, one_before):
    line, low, high, low_x, high_y = blocks
    low_y = sent(after(jnp.concatenate([low, low_x]), three_before), by=1)
    high_x = sent(after(jnp.concatenate([high, high_y]), three_before), bx=1)
    near = jnp.concatenate([line, low_x, high_y])
    far = [after(block, one_before) for block in (low_y, high_x)]
    return [near, low_y, high_x] + [sent(block, bc=1) for block in (near, *far)]


def gathered_ids():
    tp = lax.axis_size("tp")
    columns = lax.axis_size("sp") // 4
    low, high = range(columns // 4), range(columns // 4, columns)
    own = [(d, 0, 0) for d in range(columns)] + [(d, 1, 0) for d in low] + [(d, 0, 1) for d in high]
    own += [(d, bx, 1) for bx in (0, 1) for d in low]
    own += [(d, 1, by) for by in (0, 1) for d in high]
    s, y = lax.axis_index("sp"), lax.axis_index("tp")
    dz, bx, by, bc = (jnp.array(v, jnp.int32) for v in zip(*[(*p, c) for c in (0, 1) for p in own]))
    z = (s // 4 - dz) % columns
    return jnp.stack([z * 4 + (s // 2 % 2 ^ bx) * 2 + (s % 2 ^ bc), y ^ by, jnp.full(dz.shape, y)])


def split_tokens(stream, norm_gain, in_weight, out_weight, docs):
    length = stream.shape[1]
    own_len = length // 2
    half = lax.axis_index("tp")
    first = half == 0
    swap = lambda a: sent(a, by=1)
    ids = gathered_ids()

    middle = stream[:, own_len - HALO:own_len]
    other_gain = swap(norm_gain)
    docs_before = passed_along(docs[length - HALO:] + 1, "sp", 1)
    asked = lax.dynamic_slice_in_dim(stream, (1 - half) * own_len, own_len, axis=1)
    shards = [block[layer] for layer in range(LAYERS) for block in (in_weight, out_weight)]
    asked, shards[0], other_gain, docs_before = lax.optimization_barrier(
        (asked, shards[0], other_gain, docs_before))
    theirs = swap(asked)
    ours = lax.dynamic_slice_in_dim(stream, half * own_len, own_len, axis=1)

    weights, line = [], None
    for shard in shards:
        if line is not None:
            shard, line = lax.optimization_barrier((shard, line))
            weights.append(spread(line))
        line = lined_up(shard)
    weights.append(spread(line))

    before = passed_along(stream[:, length - HALO:], "sp", 1)
    our_edge = jnp.where(first, before, middle)
    their_edge = swap(jnp.where(first, middle, before))
    ext_docs = jnp.concatenate([docs_before, docs + 1])
    span = own_len + HALO
    ours = jnp.concatenate([our_edge, ours], axis=1)
    theirs = jnp.concatenate([their_edge, theirs], axis=1)
    x = jnp.concatenate([jnp.where(first, ours, theirs), jnp.where(first, theirs, ours)], axis=0)
    marks = lax.dynamic_slice_in_dim(ext_docs, half * own_len, span)[None, :]
    gain = jnp.concatenate([jnp.where(first, norm_gain, other_gain), jnp.where(first, other_gain, norm_gain)], axis=1)

    done = [None, None, None]
    for layer in range(LAYERS):
        in_parts = spread_on(weights[2 * layer], done[-3], done[-1])
        pooled = call(
            functools.partial(in_kernel, parts=len(in_parts)),
            jax.ShapeDtypeStruct((PW, span), jnp.bfloat16),
            ids, (x, gain[layer][:, None], marks), in_parts, (D, PW))
        done.append(pooled)
        out_parts = spread_on(weights[2 * layer + 1], done[-3], done[-1])
        if layer < LAYERS - 1:
            x = call(
                functools.partial(out_kernel, parts=len(out_parts), skip=0, flip=None),
                jax.ShapeDtypeStruct((D, span), jnp.float32),
                ids, (x, pooled), out_parts, (PW, D))
            done.append(x)
    given, kept = [call(
        functools.partial(out_kernel, parts=len(out_parts), skip=HALO, flip=flip),
        jax.ShapeDtypeStruct((D // 2, own_len), jnp.bfloat16),
        ids, (x, pooled), out_parts, (PW, D)) for flip in (1, 0)]
    got = swap(given)
    out = jnp.zeros((D // 2, length), jnp.bfloat16)
    out = lax.dynamic_update_slice_in_dim(out, kept, half * own_len, axis=1)
    return lax.dynamic_update_slice_in_dim(out, got, (1 - half) * own_len, axis=1)


def per_device(stream, norm_gain, in_weight, out_weight, docs):
    tokens_fit = lax.axis_size("tp") == 2 and lax.axis_size("sp") % 16 == 0 and stream.shape[1] % 256 == 0
    plan = split_tokens if tokens_fit else split_channels
    return plan(stream, norm_gain, in_weight, out_weight, docs)


def solution(mesh):
    return jax.shard_map(
        per_device,
        mesh=mesh,
        in_specs=(P("tp", "sp"), P(None, "tp"), P(None, "sp", "tp"), P(None, "tp", "sp"), P("sp")),
        out_specs=P("tp", "sp"),
        check_vma=False,
    )
```
